32 devices in a mesh: fs: 4 (over z), rep: 4 (over y, x), tp: 2 (over core).
Axes of the slice: x: 2, y: 2, z: 4, core: 2. Of those that a mesh axis runs over, the one named last changes fastest.
Arguments:
- saved_latent: bfloat16 [12288, 2048], P(('fs', 'rep')), may hold values from -6 to 6
- query_cotangent: bfloat16 [12288, 3072], P(('fs', 'rep'), 'tp'), may hold values from -6 to 6
- mix_cotangent: bfloat16 [12288, 4096], P(('fs', 'rep')), may hold values from -6 to 6
- head_outputs: bfloat16 [12288, 2048], P(('fs', 'rep'), 'tp'), may hold values from -6 to 6
- query_weight: float32 [2048, 3072], P('fs', 'tp'), may hold values from -0.125 to 0.125
- out_weight: float32 [4096, 2048], P('fs', 'tp'), may hold values from -0.125 to 0.125
- query_basis: bfloat16 [2048, 256], replicated, may hold values from -0.125 to 0.125
- out_basis: bfloat16 [4096, 256], replicated, may hold values from -0.09375 to 0.09375
- query_mean: float32 [256, 3072], P('fs', 'tp'), may hold values from -3 to 3
- query_var: float32 [256, 3072], P('fs', 'tp'), may hold values from 0.1 to 1
- out_mean: float32 [256, 2048], P('fs', 'tp'), may hold values from -3 to 3
- out_var: float32 [256, 2048], P('fs', 'tp'), may hold values from 0.1 to 1
Outputs:
- query_step: float32 [2048, 3072], P('fs', 'tp')
- out_step: float32 [4096, 2048], P('fs', 'tp')
- query_copy: bfloat16 [2048, 3072], P('fs', 'tp')
- out_copy: bfloat16 [4096, 2048], P('fs', 'tp')
The draws below stay inside these ranges and needn't reach their ends.
All inputs are finite; a program needn't handle non-finite values.
Results may differ from the reference program's by a relative error of at most 0.001.
Values sent between devices are 32-bit elements; how exact they have to be, the bound alone decides.
A program may use at most 128 MiB of HBM per device.

```python
import math
import jax
import jax.numpy as jnp
from jax import lax

D = 4096
QLORA = 2048
RANK = 256
TOKENS = 12288
QCOLS = 3072
HV = 2048


def block_scale(key, shape, shards, smallest, largest):
    loudness, own = 1.0, jax.random.fold_in(key, 6)
    for position, shards_of in shards:
        draws = jnp.exp(jax.random.uniform(jax.random.fold_in(own, position), (shards_of,), jnp.float32, smallest / len(shards), largest / len(shards)))
        loudness = loudness * jnp.repeat(draws, shape[position] // shards_of).reshape([-1 if axis == position else 1 for axis in range(len(shape))])
    return loudness


def noise(own_key, dims, deviation, limit, cuts=(), kind=jnp.bfloat16):
    drawn = jax.random.normal(own_key, dims, jnp.float32) * deviation
    if len(cuts) > 0:
        drawn = block_scale(own_key, dims, cuts, -0.22, 0.18) * drawn
    return jnp.clip(drawn, min=-limit, max=limit).astype(kind)


def setup_inputs(seed: int = 0) -> dict:
    streams_of = jax.random.split(jax.random.key(seed), 13)
    saved_latent = noise(streams_of[0], (TOKENS, QLORA), 1.0, 6.0, ((0, 16),))
    query_cotangent = noise(streams_of[1], (TOKENS, QCOLS), 1.0, 6.0, ((0, 16), (1, 2)))
    mix_cotangent = noise(streams_of[2], (TOKENS, D), 1.0, 6.0, ((0, 16),))
    head_outputs = noise(streams_of[3], (TOKENS, HV), 1.0, 6.0, ((0, 16), (1, 2)))
    query_weight = noise(streams_of[4], (QLORA, QCOLS), QLORA ** -0.5, 0.125, ((0, 4), (1, 2)), jnp.float32)
    out_weight = noise(streams_of[5], (D, HV), HV ** -0.5, 0.125, ((0, 4), (1, 2)), jnp.float32)
    query_basis = noise(streams_of[6], (QLORA, RANK), QLORA ** -0.5, 0.125)
    out_basis = noise(streams_of[7], (D, RANK), D ** -0.5, 0.09375)
    query_mean = noise(streams_of[8], (RANK, QCOLS), 0.5, 3.0, ((0, 4), (1, 2)), jnp.float32)
    query_var = jnp.clip(jnp.exp(math.log(1.0) - 2.3025851 * jax.random.uniform(streams_of[9], (RANK, QCOLS), jnp.float32) ** block_scale(streams_of[9], (RANK, QCOLS), ((0, 4), (1, 2)), -0.2, 0.2)), 0.1, 1.0)
    out_mean = noise(streams_of[10], (RANK, HV), 0.5, 3.0, ((0, 4), (1, 2)), jnp.float32)
    out_var = jnp.clip(jnp.exp(math.log(1.0) - 2.3025851 * jax.random.uniform(streams_of[11], (RANK, HV), jnp.float32) ** block_scale(streams_of[11], (RANK, HV), ((0, 4), (1, 2)), -0.2, 0.2)), 0.1, 1.0)
    return dict(saved_latent=saved_latent, query_cotangent=query_cotangent, mix_cotangent=mix_cotangent, head_outputs=head_outputs, query_weight=query_weight, out_weight=out_weight, query_basis=query_basis, out_basis=out_basis, query_mean=query_mean, query_var=query_var, out_mean=out_mean, out_var=out_var)


def token_sum(left, right):
    return lax.dot_general(left, right, (((0,), (0,)), ((), ())), preferred_element_type=jnp.float32)

def project(basis, grad):
    return lax.dot_general(basis.astype(jnp.float32), grad, (((0,), (0,)), ((), ())), precision=lax.Precision.HIGHEST)

def moment_direction(proj, mean, var):
    scale = 1.0 / jnp.maximum(jnp.sqrt(jnp.mean(proj * proj)), 1.0)
    scaled = scale * proj
    new_mean = 0.8 * mean + 0.2 * scaled
    new_var = 0.9 * var + 0.1 * scaled * scaled
    return new_mean / jnp.sqrt(new_var)

def reference(saved_latent, query_cotangent, mix_cotangent, head_outputs, query_weight, out_weight, query_basis, out_basis, query_mean, query_var, out_mean, out_var):
    query_grad = token_sum(saved_latent, query_cotangent)
    out_grad = token_sum(mix_cotangent, head_outputs)
    query_dir = moment_direction(project(query_basis, query_grad), query_mean, query_var)
    out_dir = moment_direction(project(out_basis, out_grad), out_mean, out_var)
    query_step = jnp.dot(query_basis.astype(jnp.float32), query_dir, precision=lax.Precision.HIGHEST)
    out_step = jnp.dot(out_basis.astype(jnp.float32), out_dir, precision=lax.Precision.HIGHEST)
    query_copy = (query_weight - 0.05 * query_step).astype(jnp.bfloat16)
    out_copy = (out_weight - 0.05 * out_step).astype(jnp.bfloat16)
    return (query_step, out_step, query_copy, out_copy)
```

```python
import functools

import jax
import jax.numpy as jnp
from jax import lax
from jax.experimental import pallas as pl
from jax.experimental.pallas import tpu as pltpu
from jax.sharding import PartitionSpec as P

MESH = pl.DeviceIdType.MESH
REP = 4


def flip(r, bits):
    if bits == 1:
        return r + 1 - 2 * lax.rem(r, 2)
    if bits == 2:
        return lax.rem(r + 2, REP)
    return REP - 1 - r


class Stream:
    def __init__(self, names, refs):
        self.__dict__.update(zip(names, refs))


STREAM_IN = ("left_hbm", "right_hbm", "basis_hbm", "mean_hbm", "var_hbm")
STREAM_SCRATCH = (
    "left", "right", "basis", "mean", "var", "pair", "part", "fwd_in", "keep_in", "last_in",
    "row_in", "near", "far",
)


def exchange_kernel(n_f, n_t, n_sem, *refs):
    ins, outs, scratch = refs[:10], refs[10:12], refs[12:]
    streams = []
    per = len(STREAM_SCRATCH)
    for i in range(2):
        s = Stream(STREAM_IN, ins[5 * i : 5 * i + 5])
        s.__dict__.update(zip(STREAM_SCRATCH, scratch[per * i : per * i + per]))
        s.gathered = outs[i]
        s.width = s.part.shape[-1]
        streams.append(s)
    load_sem, send_sem, recv_sem = scratch[2 * per :]
    f, r, t = lax.axis_index("fs"), lax.axis_index("rep"), lax.axis_index("tp")
    rank = streams[0].gathered.shape[1]
    rows = rank // n_f
    half = rows // 2
    counter = [0]
    pending = []

    def send(src, dst, where):
        k = counter[0]
        counter[0] += 1
        copy = pltpu.make_async_remote_copy(
            src_ref=src, dst_ref=dst, send_sem=send_sem.at[k], recv_sem=recv_sem.at[k],
            device_id=where, device_id_type=MESH,
        )
        copy.start()
        pending.append(copy)
        return copy

    loads = {}
    slot = 0
    for i, s in enumerate(streams):
        cols = pl.ds(pl.multiple_of(r * s.width, 128), s.width)
        for name in ("basis", "left", "right", "mean", "var"):
            src = getattr(s, name + "_hbm")
            if name in ("mean", "var"):
                src = src.at[:, cols]
            copy = pltpu.make_async_copy(src, getattr(s, name), load_sem.at[slot])
            copy.start()
            loads[i, name] = copy
            slot += 1

    group = n_t * REP
    place = r * n_t + t

    def neighbour(k):
        other = lax.rem(place + k, group)
        return {"rep": other // n_t, "tp": lax.rem(other, n_t)}

    barrier = pltpu.get_barrier_semaphore()
    for k in range(1, group):
        pl.semaphore_signal(barrier, inc=1, device_id=neighbour(k), device_id_type=MESH)
    for k in range(1, n_f):
        pl.semaphore_signal(
            barrier, inc=1, device_id={"fs": lax.rem(f + k, n_f)}, device_id_type=MESH
        )

    def token_product(i, s):
        loads[i, "basis"].wait()
        loads[i, "left"].wait()
        tokens = s.left.shape[0]
        step = 256

        @pl.loop(0, tokens // step)
        def _(b):
            at = pl.ds(pl.multiple_of(b * step, step), step)
            turned = jnp.dot(s.left[at, :], s.basis[...], preferred_element_type=jnp.float32).T
            high = turned.astype(jnp.bfloat16)
            s.pair[:rank, at] = high
            s.pair[rank:, at] = (turned - high.astype(jnp.float32)).astype(jnp.bfloat16)

    def quarter(s, c):
        cols = pl.ds(pl.multiple_of(c * s.width, 128), s.width)
        both = jnp.dot(s.pair[...], s.right[:, cols], preferred_element_type=jnp.float32)
        value = both[:rank] + both[rank:]
        for g in range(n_f):
            for h in range(2):
                start = g * rows + h * half
                s.part[h, c, g] = value[start : start + half]

    first = (1, 2)
    second = (2, 1)

    def partials(i, s):
        token_product(i, s)
        loads[i, "right"].wait()
        quarter(s, flip(r, 3))
        if i == 0:
            pl.semaphore_wait(barrier, group - 1 + n_f - 1)
        s.fwd, s.keep = [], [None, None]
        for h in range(2):
            s.fwd.append(
                send(s.part.at[h, flip(r, 3)], s.fwd_in.at[h], {"rep": flip(r, first[h])})
            )
        for h in range(2):
            quarter(s, flip(r, first[h]))
            s.keep[h] = send(
                s.part.at[h, flip(r, first[h])], s.keep_in.at[h], {"rep": flip(r, first[h])}
            )
        quarter(s, r)

    def forward(s):
        s.last = []
        for h in range(2):
            s.fwd[h].wait_recv()
            c = flip(r, second[h])
            s.part[h, c] = s.part[h, c] + s.fwd_in[h]
            s.last.append(send(s.part.at[h, c], s.last_in.at[h], {"rep": c}))

    def scatter_rows(s):
        s.row = {}
        for h in range(2):
            s.keep[h].wait_recv()
            s.last[h].wait_recv()
            s.part[h, r] = s.part[h, r] + s.keep_in[h] + s.last_in[h]
            for k in range(1, n_f):
                g = lax.rem(f + k, n_f)
                s.row[k, h] = send(s.part.at[h, r, g], s.row_in.at[k - 1, h], {"fs": g})

    def squares(s):
        total = jnp.zeros((8, 128), jnp.float32)
        for h in range(2):
            value = s.part[h, r, f]
            for k in range(1, n_f):
                s.row[k, h].wait_recv()
                value = value + s.row_in[k - 1, h]
            s.part[h, r, f] = value
            square = value * value
            for a in range(half // 8):
                for b in range(s.width // 128):
                    total = total + square[a * 8 : a * 8 + 8, b * 128 : b * 128 + 128]
        s.near[place] = total
        s.near_copies = [
            send(s.near.at[place], s.near.at[place], neighbour(k)) for k in range(1, group)
        ]

    def squares_far(s):
        for copy in s.near_copies:
            copy.wait_recv()
        s.far[f] = jnp.sum(s.near[...], axis=0)
        s.far_copies = [
            send(s.far.at[f], s.far.at[f], {"fs": lax.rem(f + k, n_f)}) for k in range(1, n_f)
        ]

    def direction(i, s):
        loads[i, "mean"].wait()
        loads[i, "var"].wait()
        for copy in s.far_copies:
            copy.wait_recv()
        total = jnp.sum(jnp.sum(s.far[...], axis=0), keepdims=True)
        count = float(rank * s.width * REP * n_t)
        scale = 1.0 / jnp.maximum(jnp.sqrt(total / count), 1.0)
        for h in range(2):
            scaled = scale * s.part[h, r, f]
            at = slice(h * half, (h + 1) * half)
            new_mean = 0.8 * s.mean[at, :] + 0.2 * scaled
            new_var = 0.9 * s.var[at, :] + 0.1 * scaled * scaled
            rank_rows = pl.ds(pl.multiple_of(f * rows + h * half, 8), half)
            s.gathered[r, rank_rows, :] = new_mean / jnp.sqrt(new_var)
        own = s.gathered.at[r, pl.ds(pl.multiple_of(f * rows, 8), rows), :]
        s.ring = {k: send(own, own, {"fs": lax.rem(f + k, n_f)}) for k in range(1, n_f)}
        s.side = {}

    order = sorted(range(n_f), key=lambda k: min(k, n_f - k))

    def piece(s, c, k, h):
        g = lax.rem(f + n_f - k, n_f)
        return s.gathered.at[c, pl.ds(pl.multiple_of(g * rows + h * half, 8), half), :]

    def spread_one(s, k):
        if k > 0:
            s.ring[k].wait_recv()
        for h in range(2):
            own = piece(s, r, k, h)
            s.side[k, h] = send(own, own, {"rep": flip(r, second[h])})
        for h in range(2):
            own = piece(s, r, k, h)
            s.side[k, h, "own"] = send(own, own, {"rep": flip(r, first[h])})

    def spread_two(s, k):
        for h in range(2):
            s.side[k, h].wait_recv()
            passed = piece(s, flip(r, second[h]), k, h)
            s.side[k, h, "pass"] = send(passed, passed, {"rep": flip(r, first[h])})

    q, o = streams
    partials(0, q)
    forward(q)
    partials(1, o)
    scatter_rows(q)
    forward(o)
    squares(q)
    scatter_rows(o)
    squares_far(q)
    direction(0, q)
    squares(o)
    squares_far(o)
    spread_one(q, 0)
    direction(1, o)
    for j, k in enumerate(order):
        if j > 0:
            spread_one(q, k)
            spread_two(q, order[j - 1])
    spread_one(o, 0)
    spread_two(q, order[-1])
    for j, k in enumerate(order):
        if j > 0:
            spread_one(o, k)
            spread_two(o, order[j - 1])
    spread_two(o, order[-1])
    for s in streams:
        for k in range(n_f):
            for h in range(2):
                s.side[k, h, "own"].wait_recv()
                s.side[k, h, "pass"].wait_recv()
    for copy in pending:
        copy.wait_send()


def step_kernel(_, *refs):
    for i in range(2):
        basis, moved, weight = refs[3 * i : 3 * i + 3]
        step_ref, copy_ref = refs[6 + 2 * i : 8 + 2 * i]
        value = moved[0]
        high = value.astype(jnp.bfloat16)
        low = (value - high.astype(jnp.float32)).astype(jnp.bfloat16)
        step = jnp.dot(basis[...], high, preferred_element_type=jnp.float32) + jnp.dot(
            basis[...], low, preferred_element_type=jnp.float32
        )
        step_ref[...] = step
        copy_ref[...] = (weight[...] - 0.05 * step).astype(jnp.bfloat16)


def on_device(
    n_f, n_t,
    saved_latent, query_cotangent, mix_cotangent, head_outputs, query_weight, out_weight,
    query_basis, out_basis, query_mean, query_var, out_mean, out_var,
):
    f32, bf16 = jnp.float32, jnp.bfloat16
    rank = query_basis.shape[1]
    rows = rank // n_f
    half = rows // 2
    groups = (
        (saved_latent, query_cotangent, query_basis, query_mean, query_var),
        (mix_cotangent, head_outputs, out_basis, out_mean, out_var),
    )
    scratch, outs = [], []
    for left, right, basis, mean, _ in groups:
        w = right.shape[1] // REP
        scratch += [
            pltpu.VMEM(left.shape, bf16),
            pltpu.VMEM(right.shape, bf16),
            pltpu.VMEM(basis.shape, bf16),
            pltpu.VMEM((rows, w), f32),
            pltpu.VMEM((rows, w), f32),
            pltpu.VMEM((2 * rank, left.shape[0]), bf16),
            pltpu.VMEM((2, REP, n_f, half, w), f32),
            pltpu.VMEM((2, n_f, half, w), f32),
            pltpu.VMEM((2, n_f, half, w), f32),
            pltpu.VMEM((2, n_f, half, w), f32),
            pltpu.VMEM((n_f - 1, 2, half, w), f32),
            pltpu.VMEM((REP * n_t, 8, 128), f32),
            pltpu.VMEM((n_f, 8, 128), f32),
        ]
        outs.append(jax.ShapeDtypeStruct((REP, rank, w), f32))
    n_sem = 2 * (6 + 2 * (n_f - 1) + REP * n_t - 1 + (n_f - 1) + (n_f - 1) + 6 * n_f)
    moved_query, moved_out = pl.pallas_call(
        functools.partial(exchange_kernel, n_f, n_t, n_sem),
        out_shape=outs,
        in_specs=[pl.BlockSpec(memory_space=pl.ANY)] * 10,
        out_specs=[pl.BlockSpec(memory_space=pltpu.VMEM)] * 2,
        scratch_shapes=scratch
        + [
            pltpu.SemaphoreType.DMA((10,)),
            pltpu.SemaphoreType.DMA((n_sem,)),
            pltpu.SemaphoreType.DMA((n_sem,)),
        ],
        compiler_params=pltpu.CompilerParams(
            collective_id=0, has_side_effects=True, vmem_limit_bytes=48 * 1024 * 1024
        ),
        name="exchange",
    )(*groups[0], *groups[1])

    cuts = 2
    specs_in, specs_out, shapes = [], [], []
    for weight, basis, moved in (
        (query_weight, query_basis, moved_query),
        (out_weight, out_basis, moved_out),
    ):
        w = moved.shape[2]
        high = weight.shape[0] // cuts
        block = pl.BlockSpec((high, w), lambda c, b, at: (b, c))
        specs_in += [
            pl.BlockSpec((high, rank), lambda c, b, at: (at[0] * cuts + b, 0)),
            pl.BlockSpec((1, rank, w), lambda c, b, at: (c, 0, 0)),
            block,
        ]
        specs_out += [block, block]
        shapes += [
            jax.ShapeDtypeStruct(weight.shape, f32),
            jax.ShapeDtypeStruct(weight.shape, bf16),
        ]
    position = lax.axis_index("fs").astype(jnp.int32).reshape(1)
    query_step, query_copy, out_step, out_copy = pl.pallas_call(
        step_kernel,
        out_shape=shapes,
        grid_spec=pltpu.PrefetchScalarGridSpec(
            num_scalar_prefetch=1, grid=(REP, cuts), in_specs=specs_in, out_specs=specs_out
        ),
        compiler_params=pltpu.CompilerParams(
            dimension_semantics=("arbitrary", "arbitrary"), vmem_limit_bytes=32 * 1024 * 1024
        ),
        name="steps",
    )(position, query_basis, moved_query, query_weight, out_basis, moved_out, out_weight)
    return query_step, out_step, query_copy, out_copy


def solution(mesh):
    sizes = dict(mesh.shape)
    assert sizes["rep"] == REP
    placed = (
        P(("fs", "rep"), None),
        P(("fs", "rep"), "tp"),
        P(("fs", "rep"), None),
        P(("fs", "rep"), "tp"),
        P("fs", "tp"),
        P("fs", "tp"),
        P(),
        P(),
        P("fs", "tp"),
        P("fs", "tp"),
        P("fs", "tp"),
        P("fs", "tp"),
    )
    return jax.shard_map(
        functools.partial(on_device, sizes["fs"], sizes["tp"]),
        mesh=mesh,
        in_specs=placed,
        out_specs=(P("fs", "tp"), P("fs", "tp"), P("fs", "tp"), P("fs", "tp")),
        check_vma=False,
    )
```

```python
import functools

import jax
import jax.numpy as jnp
from jax import lax
from jax.experimental import pallas as pl
from jax.experimental.pallas import tpu as pltpu
from jax.sharding import PartitionSpec as P

MESH = pl.DeviceIdType.MESH
REP = 4
LANES = 128
TOKEN_STEP = 256


def flip(r, bits):
    if bits == 1:
        return r + 1 - 2 * lax.rem(r, 2)
    if bits == 2:
        return lax.rem(r + 2, REP)
    return REP - 1 - r


class Stream:
    def __init__(self, names, refs):
        self.__dict__.update(zip(names, refs))


STREAM_IN = ("left_hbm", "right_hbm", "basis_hbm", "mean_hbm", "var_hbm")
STREAM_SCRATCH = (
    "left", "right", "basis", "mean", "var", "pair", "part", "fwd_in", "keep_in", "last_in",
    "row_in", "near", "far",
)


def exchange_kernel(n_f, n_t, n_sem, *refs):
    ins, outs, scratch = refs[:10], refs[10:12], refs[12:]
    streams = []
    per = len(STREAM_SCRATCH)
    for i in range(2):
        s = Stream(STREAM_IN, ins[5 * i : 5 * i + 5])
        s.__dict__.update(zip(STREAM_SCRATCH, scratch[per * i : per * i + per]))
        s.gathered = outs[i]
        s.width = s.gathered.shape[-1]
        s.pieces = s.width // LANES
        streams.append(s)
    load_sem, send_sem, recv_sem = scratch[2 * per :]
    f, r, t = lax.axis_index("fs"), lax.axis_index("rep"), lax.axis_index("tp")
    rank = streams[0].gathered.shape[1]
    rows = rank // n_f
    half = rows // 2
    counter = [0]
    pending = []

    def send(src, dst, where):
        k = counter[0]
        counter[0] += 1
        copy = pltpu.make_async_remote_copy(
            src_ref=src, dst_ref=dst, send_sem=send_sem.at[k], recv_sem=recv_sem.at[k],
            device_id=where, device_id_type=MESH,
        )
        copy.start()
        pending.append(copy)
        return copy

    loads = {}
    slot = 0
    for i, s in enumerate(streams):
        cols = pl.ds(pl.multiple_of(r * s.width, 128), s.width)
        blocks = s.left.shape[0] // TOKEN_STEP
        for name in ["basis", *range(blocks), "right", "mean", "var"]:
            if name in ("mean", "var"):
                src, dst = getattr(s, name + "_hbm").at[:, cols], getattr(s, name)
            elif name in ("basis", "right"):
                src, dst = getattr(s, name + "_hbm"), getattr(s, name)
            else:
                at = pl.ds(name * TOKEN_STEP, TOKEN_STEP)
                src, dst = s.left_hbm.at[at, :], s.left.at[at, :]
            copy = pltpu.make_async_copy(src, dst, load_sem.at[slot])
            copy.start()
            loads[i, name] = copy
            slot += 1

    group = n_t * REP
    place = r * n_t + t

    def neighbour(k):
        other = lax.rem(place + k, group)
        return {"rep": other // n_t, "tp": lax.rem(other, n_t)}

    barrier = pltpu.get_barrier_semaphore()
    for k in range(1, group):
        pl.semaphore_signal(barrier, inc=1, device_id=neighbour(k), device_id_type=MESH)
    for k in range(1, n_f):
        pl.semaphore_signal(
            barrier, inc=1, device_id={"fs": lax.rem(f + k, n_f)}, device_id_type=MESH
        )

    def token_product(i, s, b):
        if b == 0:
            loads[i, "basis"].wait()
        loads[i, b].wait()
        at = slice(b * TOKEN_STEP, (b + 1) * TOKEN_STEP)
        turned = jnp.dot(s.left[at, :], s.basis[...], preferred_element_type=jnp.float32).T
        high = turned.astype(jnp.bfloat16)
        s.pair[:rank, at] = high
        s.pair[rank:, at] = (turned - high.astype(jnp.float32)).astype(jnp.bfloat16)

    def quarter(s, c):
        cols = pl.ds(pl.multiple_of(c * s.width, LANES), s.width)
        both = jnp.dot(s.pair[...], s.right[:, cols], preferred_element_type=jnp.float32)
        value = both[:rank] + both[rank:]
        for g in range(n_f):
            for h in range(2):
                start = g * rows + h * half
                for p in range(s.pieces):
                    s.part[h, c, p, g] = value[start : start + half, p * LANES : (p + 1) * LANES]

    first = (1, 2)
    second = (2, 1)

    def send_fwd(s, p):
        for h in range(2):
            s.fwd[h, p] = send(
                s.part.at[h, flip(r, 3), p], s.fwd_in.at[h, p], {"rep": flip(r, first[h])}
            )

    def send_keep(s, p):
        for h in range(2):
            c = flip(r, first[h])
            s.keep[h, p] = send(s.part.at[h, c, p], s.keep_in.at[h, p], {"rep": c})

    def forward(s, p):
        for h in range(2):
            s.fwd[h, p].wait_recv()
            c = flip(r, second[h])
            s.part[h, c, p] = s.part[h, c, p] + s.fwd_in[h, p]
            s.last[h, p] = send(s.part.at[h, c, p], s.last_in.at[h, p], {"rep": c})

    def scatter_rows(s, p):
        for h in range(2):
            s.keep[h, p].wait_recv()
            s.last[h, p].wait_recv()
            s.part[h, r, p] = s.part[h, r, p] + s.keep_in[h, p] + s.last_in[h, p]
            for k in range(1, n_f):
                g = lax.rem(f + k, n_f)
                s.row[k, h, p] = send(
                    s.part.at[h, r, p, g], s.row_in.at[k - 1, h, p], {"fs": g}
                )

    def squares(s):
        total = jnp.zeros((8, 128), jnp.float32)
        for p in range(s.pieces):
            for h in range(2):
                value = s.part[h, r, p, f]
                for k in range(1, n_f):
                    s.row[k, h, p].wait_recv()
                    value = value + s.row_in[k - 1, h, p]
                s.part[h, r, p, f] = value
                square = value * value
                for a in range(half // 8):
                    total = total + square[a * 8 : a * 8 + 8]
        s.near[place] = total
        s.near_copies = [
            send(s.near.at[place], s.near.at[place], neighbour(k)) for k in range(1, group)
        ]

    def squares_far(s):
        for copy in s.near_copies:
            copy.wait_recv()
        s.far[f] = jnp.sum(s.near[...], axis=0)
        s.far_copies = [
            send(s.far.at[f], s.far.at[f], {"fs": lax.rem(f + k, n_f)}) for k in range(1, n_f)
        ]

    def direction(i, s):
        loads[i, "mean"].wait()
        loads[i, "var"].wait()
        for copy in s.far_copies:
            copy.wait_recv()
        total = jnp.sum(jnp.sum(s.far[...], axis=0), keepdims=True)
        count = float(rank * s.width * REP * n_t)
        scale = 1.0 / jnp.maximum(jnp.sqrt(total / count), 1.0)
        for h in range(2):
            at = slice(h * half, (h + 1) * half)
            rank_rows = pl.ds(pl.multiple_of(f * rows + h * half, 8), half)
            for p in range(s.pieces):
                cols = slice(p * LANES, (p + 1) * LANES)
                scaled = scale * s.part[h, r, p, f]
                new_mean = 0.8 * s.mean[at, cols] + 0.2 * scaled
                new_var = 0.9 * s.var[at, cols] + 0.1 * scaled * scaled
                s.gathered[r, rank_rows, cols] = new_mean / jnp.sqrt(new_var)
        own = s.gathered.at[r, pl.ds(pl.multiple_of(f * rows, 8), rows), :]
        s.ring = {k: send(own, own, {"fs": lax.rem(f + k, n_f)}) for k in range(1, n_f)}
        s.side = {}

    order = sorted(range(n_f), key=lambda k: min(k, n_f - k))

    def piece(s, c, k, h):
        g = lax.rem(f + n_f - k, n_f)
        return s.gathered.at[c, pl.ds(pl.multiple_of(g * rows + h * half, 8), half), :]

    def spread_one(s, k):
        if k > 0:
            s.ring[k].wait_recv()
        for h in range(2):
            own = piece(s, r, k, h)
            s.side[k, h] = send(own, own, {"rep": flip(r, second[h])})
        for h in range(2):
            own = piece(s, r, k, h)
            s.side[k, h, "own"] = send(own, own, {"rep": flip(r, first[h])})

    def spread_two(s, k):
        for h in range(2):
            s.side[k, h].wait_recv()
            passed = piece(s, flip(r, second[h]), k, h)
            s.side[k, h, "pass"] = send(passed, passed, {"rep": flip(r, first[h])})

    q, o = streams
    for s in streams:
        s.fwd, s.keep, s.last, s.row = {}, {}, {}, {}
    blocks = q.left.shape[0] // TOKEN_STEP
    for b in range(blocks):
        token_product(0, q, b)
    loads[0, "right"].wait()
    quarter(q, flip(r, 3))
    pl.semaphore_wait(barrier, group - 1 + n_f - 1)
    send_fwd(q, 0)
    quarter(q, flip(r, 1))
    quarter(q, flip(r, 2))
    send_keep(q, 0)
    for p in range(1, q.pieces - 1):
        send_fwd(q, p)
        send_keep(q, p)
    quarter(q, r)
    token_product(1, o, 0)
    forward(q, 0)
    send_fwd(q, q.pieces - 1)
    send_keep(q, q.pieces - 1)
    for b in range(1, blocks):
        token_product(1, o, b)
    for p in range(1, q.pieces - 1):
        forward(q, p)
    loads[1, "right"].wait()
    quarter(o, flip(r, 3))
    quarter(o, flip(r, 1))
    quarter(o, flip(r, 2))
    scatter_rows(q, 0)
    forward(q, q.pieces - 1)
    for p in range(o.pieces):
        send_fwd(o, p)
        send_keep(o, p)
    quarter(o, r)
    for p in range(1, q.pieces):
        scatter_rows(q, p)
    for p in range(o.pieces):
        forward(o, p)
    squares(q)
    scatter_rows(o, 0)
    squares_far(q)
    for p in range(1, o.pieces):
        scatter_rows(o, p)
    direction(0, q)
    spread_one(q, 0)
    squares(o)
    squares_far(o)
    direction(1, o)
    for j, k in enumerate(order):
        if j > 0:
            spread_one(q, k)
            spread_two(q, order[j - 1])
    spread_one(o, 0)
    spread_two(q, order[-1])
    for j, k in enumerate(order):
        if j > 0:
            spread_one(o, k)
            spread_two(o, order[j - 1])
    spread_two(o, order[-1])
    for s in streams:
        for k in range(n_f):
            for h in range(2):
                s.side[k, h, "own"].wait_recv()
                s.side[k, h, "pass"].wait_recv()
    for copy in pending:
        copy.wait_send()


def step_kernel(_, *refs):
    for i in range(2):
        basis, moved, weight = refs[3 * i : 3 * i + 3]
        step_ref, copy_ref = refs[6 + 2 * i : 8 + 2 * i]
        value = moved[0]
        high = value.astype(jnp.bfloat16)
        low = (value - high.astype(jnp.float32)).astype(jnp.bfloat16)
        step = jnp.dot(basis[...], high, preferred_element_type=jnp.float32) + jnp.dot(
            basis[...], low, preferred_element_type=jnp.float32
        )
        step_ref[...] = step
        copy_ref[...] = (weight[...] - 0.05 * step).astype(jnp.bfloat16)


def on_device(
    n_f, n_t,
    saved_latent, query_cotangent, mix_cotangent, head_outputs, query_weight, out_weight,
    query_basis, out_basis, query_mean, query_var, out_mean, out_var,
):
    f32, bf16 = jnp.float32, jnp.bfloat16
    rank = query_basis.shape[1]
    rows = rank // n_f
    half = rows // 2
    groups = (
        (saved_latent, query_cotangent, query_basis, query_mean, query_var),
        (mix_cotangent, head_outputs, out_basis, out_mean, out_var),
    )
    scratch, outs = [], []
    for left, right, basis, mean, _ in groups:
        w = right.shape[1] // REP
        scratch += [
            pltpu.VMEM(left.shape, bf16),
            pltpu.VMEM(right.shape, bf16),
            pltpu.VMEM(basis.shape, bf16),
            pltpu.VMEM((rows, w), f32),
            pltpu.VMEM((rows, w), f32),
            pltpu.VMEM((2 * rank, left.shape[0]), bf16),
            pltpu.VMEM((2, REP, w // LANES, n_f, half, LANES), f32),
            pltpu.VMEM((2, w // LANES, n_f, half, LANES), f32),
            pltpu.VMEM((2, w // LANES, n_f, half, LANES), f32),
            pltpu.VMEM((2, w // LANES, n_f, half, LANES), f32),
            pltpu.VMEM((n_f - 1, 2, w // LANES, half, LANES), f32),
            pltpu.VMEM((REP * n_t, 8, 128), f32),
            pltpu.VMEM((n_f, 8, 128), f32),
        ]
        outs.append(jax.ShapeDtypeStruct((REP, rank, w), f32))
    pieces = sum(right.shape[1] // REP // LANES for _, right, *_ in groups)
    n_sem = pieces * (6 + 2 * (n_f - 1)) + 2 * (REP * n_t - 1 + 2 * (n_f - 1) + 6 * n_f)
    n_load = sum(4 + left.shape[0] // TOKEN_STEP for left, *_ in groups)
    moved_query, moved_out = pl.pallas_call(
        functools.partial(exchange_kernel, n_f, n_t, n_sem),
        out_shape=outs,
        in_specs=[pl.BlockSpec(memory_space=pltpu.HBM)] * 10,
        out_specs=[pl.BlockSpec(memory_space=pltpu.VMEM)] * 2,
        scratch_shapes=scratch
        + [
            pltpu.SemaphoreType.DMA((n_load,)),
            pltpu.SemaphoreType.DMA((n_sem,)),
            pltpu.SemaphoreType.DMA((n_sem,)),
        ],
        compiler_params=pltpu.CompilerParams(
            collective_id=0, has_side_effects=True, vmem_limit_bytes=48 * 1024 * 1024
        ),
        name="exchange",
    )(*(pltpu.with_memory_space_constraint(x, pltpu.HBM) for group in groups for x in group))

    cuts = 2
    specs_in, specs_out, shapes = [], [], []
    for weight, basis, moved in (
        (query_weight, query_basis, moved_query),
        (out_weight, out_basis, moved_out),
    ):
        w = moved.shape[2]
        high = weight.shape[0] // cuts
        block = pl.BlockSpec((high, w), lambda c, b, at: (b, c))
        specs_in += [
            pl.BlockSpec((high, rank), lambda c, b, at: (at[0] * cuts + b, 0)),
            pl.BlockSpec((1, rank, w), lambda c, b, at: (c, 0, 0)),
            block,
        ]
        specs_out += [block, block]
        shapes += [
            jax.ShapeDtypeStruct(weight.shape, f32),
            jax.ShapeDtypeStruct(weight.shape, bf16),
        ]
    position = lax.axis_index("fs").astype(jnp.int32).reshape(1)
    query_step, query_copy, out_step, out_copy = pl.pallas_call(
        step_kernel,
        out_shape=shapes,
        grid_spec=pltpu.PrefetchScalarGridSpec(
            num_scalar_prefetch=1, grid=(REP, cuts), in_specs=specs_in, out_specs=specs_out
        ),
        compiler_params=pltpu.CompilerParams(
            dimension_semantics=("arbitrary", "arbitrary"), vmem_limit_bytes=32 * 1024 * 1024
        ),
        name="steps",
    )(position, query_basis, moved_query, query_weight, out_basis, moved_out, out_weight)
    return query_step, out_step, query_copy, out_copy


def solution(mesh):
    sizes = dict(mesh.shape)
    assert sizes["rep"] == REP
    placed = (
        P(("fs", "rep"), None),
        P(("fs", "rep"), "tp"),
        P(("fs", "rep"), None),
        P(("fs", "rep"), "tp"),
        P("fs", "tp"),
        P("fs", "tp"),
        P(),
        P(),
        P("fs", "tp"),
        P("fs", "tp"),
        P("fs", "tp"),
        P("fs", "tp"),
    )
    return jax.shard_map(
        functools.partial(on_device, sizes["fs"], sizes["tp"]),
        mesh=mesh,
        in_specs=placed,
        out_specs=(P("fs", "tp"), P("fs", "tp"), P("fs", "tp"), P("fs", "tp")),
        check_vma=False,
    )
```

```python
import functools

import jax
import jax.numpy as jnp
from jax import lax
from jax.experimental import pallas as pl
from jax.experimental.pallas import tpu as pltpu
from jax.sharding import PartitionSpec as P

MESH = pl.DeviceIdType.MESH
REP = 4
LANES = 128
TOKEN_STEP = 256


def flip(r, bits):
    if bits == 1:
        return r + 1 - 2 * lax.rem(r, 2)
    if bits == 2:
        return lax.rem(r + 2, REP)
    return REP - 1 - r


class Stream:
    def __init__(self, names, refs):
        self.__dict__.update(zip(names, refs))


STREAM_IN = ("left_hbm", "right_hbm", "basis_hbm", "mean_hbm", "var_hbm", "weight_hbm")
STREAM_SCRATCH = (
    "left", "right", "basis", "mean", "var", "pair", "part", "fwd_in", "keep_in", "last_in",
    "row_in", "near", "far",
)


def exchange_kernel(n_f, n_t, n_sem, *refs):
    ins, outs, scratch = refs[:12], refs[12:16], refs[16:]
    streams = []
    per = len(STREAM_SCRATCH)
    for i in range(2):
        s = Stream(STREAM_IN, ins[6 * i : 6 * i + 6])
        s.__dict__.update(zip(STREAM_SCRATCH, scratch[per * i : per * i + per]))
        s.gathered, s.weight = outs[i], outs[2 + i]
        s.width = s.gathered.shape[-1]
        s.pieces = s.width // LANES
        streams.append(s)
    load_sem, send_sem, recv_sem = scratch[2 * per :]
    f, r, t = lax.axis_index("fs"), lax.axis_index("rep"), lax.axis_index("tp")
    rank = streams[0].gathered.shape[1]
    rows = rank // n_f
    half = rows // 2
    counter = [0]
    pending = []

    def send(src, dst, where):
        k = counter[0]
        counter[0] += 1
        copy = pltpu.make_async_remote_copy(
            src_ref=src, dst_ref=dst, send_sem=send_sem.at[k], recv_sem=recv_sem.at[k],
            device_id=where, device_id_type=MESH,
        )
        copy.start()
        pending.append(copy)
        return copy

    loads = {}
    slots = iter(range(load_sem.shape[0]))

    def start_loads(i, s, names):
        cols = pl.ds(pl.multiple_of(r * s.width, 128), s.width)
        for name in names:
            if name in ("mean", "var"):
                src, dst = getattr(s, name + "_hbm").at[:, cols], getattr(s, name)
            elif name in ("basis", "right", "weight"):
                src, dst = getattr(s, name + "_hbm"), getattr(s, name)
            else:
                at = pl.ds(name * TOKEN_STEP, TOKEN_STEP)
                src, dst = s.left_hbm.at[at, :], s.left.at[at, :]
            copy = pltpu.make_async_copy(src, dst, load_sem.at[next(slots)])
            copy.start()
            loads[i, name] = copy

    blocks = streams[0].left.shape[0] // TOKEN_STEP
    main = ["basis", *range(blocks), "right"]
    start_loads(0, streams[0], main)

    group = n_t * REP
    place = r * n_t + t

    def neighbour(k):
        other = lax.rem(place + k, group)
        return {"rep": other // n_t, "tp": lax.rem(other, n_t)}

    barrier = pltpu.get_barrier_semaphore()
    for k in range(1, group):
        pl.semaphore_signal(barrier, inc=1, device_id=neighbour(k), device_id_type=MESH)
    for k in range(1, n_f):
        pl.semaphore_signal(
            barrier, inc=1, device_id={"fs": lax.rem(f + k, n_f)}, device_id_type=MESH
        )

    def token_product(i, s, b):
        if b == 0:
            loads[i, "basis"].wait()
        loads[i, b].wait()
        at = slice(b * TOKEN_STEP, (b + 1) * TOKEN_STEP)
        turned = jnp.dot(s.left[at, :], s.basis[...], preferred_element_type=jnp.float32).T
        high = turned.astype(jnp.bfloat16)
        s.pair[:rank, at] = high
        s.pair[rank:, at] = (turned - high.astype(jnp.float32)).astype(jnp.bfloat16)

    def quarter(s, c):
        cols = pl.ds(pl.multiple_of(c * s.width, LANES), s.width)
        both = jnp.dot(s.pair[...], s.right[:, cols], preferred_element_type=jnp.float32)
        value = both[:rank] + both[rank:]
        for g in range(n_f):
            for h in range(2):
                start = g * rows + h * half
                for p in range(s.pieces):
                    s.part[h, c, p, g] = value[start : start + half, p * LANES : (p + 1) * LANES]

    first = (1, 2)
    second = (2, 1)

    def send_fwd(s, p):
        for h in range(2):
            s.fwd[h, p] = send(
                s.part.at[h, flip(r, 3), p], s.fwd_in.at[h, p], {"rep": flip(r, first[h])}
            )

    def send_keep(s, p):
        for h in range(2):
            c = flip(r, first[h])
            s.keep[h, p] = send(s.part.at[h, c, p], s.keep_in.at[h, p], {"rep": c})

    def forward(s, p):
        for h in range(2):
            s.fwd[h, p].wait_recv()
            c = flip(r, second[h])
            s.part[h, c, p] = s.part[h, c, p] + s.fwd_in[h, p]
            s.last[h, p] = send(s.part.at[h, c, p], s.last_in.at[h, p], {"rep": c})

    def scatter_rows(s, p):
        for h in range(2):
            s.keep[h, p].wait_recv()
            s.last[h, p].wait_recv()
            s.part[h, r, p] = s.part[h, r, p] + s.keep_in[h, p] + s.last_in[h, p]
            for k in range(1, n_f):
                g = lax.rem(f + k, n_f)
                s.row[k, h, p] = send(
                    s.part.at[h, r, p, g], s.row_in.at[k - 1, h, p], {"fs": g}
                )

    def squares(s):
        total = jnp.zeros((8, 128), jnp.float32)
        for p in range(s.pieces):
            for h in range(2):
                value = s.part[h, r, p, f]
                for k in range(1, n_f):
                    s.row[k, h, p].wait_recv()
                    value = value + s.row_in[k - 1, h, p]
                s.part[h, r, p, f] = value
                square = value * value
                for a in range(half // 8):
                    total = total + square[a * 8 : a * 8 + 8]
        s.near[place] = total
        s.near_copies = [
            send(s.near.at[place], s.near.at[place], neighbour(k)) for k in range(1, group)
        ]

    def squares_far(s):
        for copy in s.near_copies:
            copy.wait_recv()
        s.far[f] = jnp.sum(s.near[...], axis=0)
        s.far_copies = [
            send(s.far.at[f], s.far.at[f], {"fs": lax.rem(f + k, n_f)}) for k in range(1, n_f)
        ]

    def direction(i, s):
        loads[i, "mean"].wait()
        loads[i, "var"].wait()
        for copy in s.far_copies:
            copy.wait_recv()
        total = jnp.sum(jnp.sum(s.far[...], axis=0), keepdims=True)
        count = float(rank * s.width * REP * n_t)
        scale = 1.0 / jnp.maximum(jnp.sqrt(total / count), 1.0)
        for h in range(2):
            at = slice(h * half, (h + 1) * half)
            rank_rows = pl.ds(pl.multiple_of(f * rows + h * half, 8), half)
            for p in range(s.pieces):
                cols = slice(p * LANES, (p + 1) * LANES)
                scaled = scale * s.part[h, r, p, f]
                new_mean = 0.8 * s.mean[at, cols] + 0.2 * scaled
                new_var = 0.9 * s.var[at, cols] + 0.1 * scaled * scaled
                s.gathered[r, rank_rows, cols] = new_mean / jnp.sqrt(new_var)
        own = s.gathered.at[r, pl.ds(pl.multiple_of(f * rows, 8), rows), :]
        s.ring = {k: send(own, own, {"fs": lax.rem(f + k, n_f)}) for k in range(1, n_f)}
        s.side = {}

    order = sorted(range(n_f), key=lambda k: min(k, n_f - k))

    def piece(s, c, k, h):
        g = lax.rem(f + n_f - k, n_f)
        return s.gathered.at[c, pl.ds(pl.multiple_of(g * rows + h * half, 8), half), :]

    def spread_one(s, k):
        if k > 0:
            s.ring[k].wait_recv()
        for h in range(2):
            own = piece(s, r, k, h)
            s.side[k, h] = send(own, own, {"rep": flip(r, second[h])})
        for h in range(2):
            own = piece(s, r, k, h)
            s.side[k, h, "own"] = send(own, own, {"rep": flip(r, first[h])})

    def spread_two(s, k):
        for h in range(2):
            s.side[k, h].wait_recv()
            passed = piece(s, flip(r, second[h]), k, h)
            s.side[k, h, "pass"] = send(passed, passed, {"rep": flip(r, first[h])})

    q, o = streams
    for s in streams:
        s.fwd, s.keep, s.last, s.row = {}, {}, {}, {}
    for b in range(blocks):
        token_product(0, q, b)
    loads[0, "right"].wait()
    start_loads(1, o, main)
    quarter(q, flip(r, 3))
    pl.semaphore_wait(barrier, group - 1 + n_f - 1)
    send_fwd(q, 0)
    quarter(q, flip(r, 1))
    quarter(q, flip(r, 2))
    send_keep(q, 0)
    for p in range(1, q.pieces - 1):
        send_fwd(q, p)
        send_keep(q, p)
    quarter(q, r)
    token_product(1, o, 0)
    forward(q, 0)
    send_fwd(q, q.pieces - 1)
    send_keep(q, q.pieces - 1)
    for b in range(1, blocks):
        token_product(1, o, b)
    for p in range(1, q.pieces - 1):
        forward(q, p)
    loads[1, "right"].wait()
    for i, s in enumerate(streams):
        start_loads(i, s, ["mean", "var", "weight"])
    quarter(o, flip(r, 3))
    quarter(o, flip(r, 1))
    quarter(o, flip(r, 2))
    scatter_rows(q, 0)
    forward(q, q.pieces - 1)
    for p in range(o.pieces):
        send_fwd(o, p)
        send_keep(o, p)
    quarter(o, r)
    for p in range(1, q.pieces):
        scatter_rows(q, p)
    for p in range(o.pieces):
        forward(o, p)
    squares(q)
    scatter_rows(o, 0)
    squares_far(q)
    for p in range(1, o.pieces):
        scatter_rows(o, p)
    direction(0, q)
    spread_one(q, 0)
    squares(o)
    spread_one(q, order[1])
    spread_two(q, order[0])
    squares_far(o)
    spread_one(q, order[2])
    spread_two(q, order[1])
    direction(1, o)
    for j in range(3, n_f):
        spread_one(q, order[j])
        spread_two(q, order[j - 1])
    spread_one(o, 0)
    spread_two(q, order[-1])
    for j in range(1, n_f):
        spread_one(o, order[j])
        spread_two(o, order[j - 1])
    spread_two(o, order[-1])
    loads[0, "weight"].wait()
    loads[1, "weight"].wait()
    for s in streams:
        for k in range(n_f):
            for h in range(2):
                s.side[k, h, "own"].wait_recv()
                s.side[k, h, "pass"].wait_recv()
    for copy in pending:
        copy.wait_send()


def step_kernel(_, *refs):
    for i in range(2):
        basis, moved, weight = refs[3 * i : 3 * i + 3]
        step_ref, copy_ref = refs[6 + 2 * i : 8 + 2 * i]
        value = moved[0]
        high = value.astype(jnp.bfloat16)
        low = (value - high.astype(jnp.float32)).astype(jnp.bfloat16)
        step = jnp.dot(basis[...], high, preferred_element_type=jnp.float32) + jnp.dot(
            basis[...], low, preferred_element_type=jnp.float32
        )
        step_ref[...] = step
        copy_ref[...] = (weight[...] - 0.05 * step).astype(jnp.bfloat16)


def on_device(
    n_f, n_t,
    saved_latent, query_cotangent, mix_cotangent, head_outputs, query_weight, out_weight,
    query_basis, out_basis, query_mean, query_var, out_mean, out_var,
):
    f32, bf16 = jnp.float32, jnp.bfloat16
    rank = query_basis.shape[1]
    rows = rank // n_f
    half = rows // 2
    groups = (
        (saved_latent, query_cotangent, query_basis, query_mean, query_var, query_weight),
        (mix_cotangent, head_outputs, out_basis, out_mean, out_var, out_weight),
    )
    scratch, outs = [], []
    for left, right, basis, *_ in groups:
        w = right.shape[1] // REP
        scratch += [
            pltpu.VMEM(left.shape, bf16),
            pltpu.VMEM(right.shape, bf16),
            pltpu.VMEM(basis.shape, bf16),
            pltpu.VMEM((rows, w), f32),
            pltpu.VMEM((rows, w), f32),
            pltpu.VMEM((2 * rank, left.shape[0]), bf16),
            pltpu.VMEM((2, REP, w // LANES, n_f, half, LANES), f32),
            pltpu.VMEM((2, w // LANES, n_f, half, LANES), f32),
            pltpu.VMEM((2, w // LANES, n_f, half, LANES), f32),
            pltpu.VMEM((2, w // LANES, n_f, half, LANES), f32),
            pltpu.VMEM((n_f - 1, 2, w // LANES, half, LANES), f32),
            pltpu.VMEM((REP * n_t, 8, 128), f32),
            pltpu.VMEM((n_f, 8, 128), f32),
        ]
        outs.append(jax.ShapeDtypeStruct((REP, rank, w), f32))
    pieces = sum(right.shape[1] // REP // LANES for _, right, *_ in groups)
    n_sem = pieces * (6 + 2 * (n_f - 1)) + 2 * (REP * n_t - 1 + 2 * (n_f - 1) + 6 * n_f)
    outs += [jax.ShapeDtypeStruct(w.shape, f32) for w in (query_weight, out_weight)]
    n_load = sum(5 + left.shape[0] // TOKEN_STEP for left, *_ in groups)
    moved_query, moved_out, near_query, near_out = pl.pallas_call(
        functools.partial(exchange_kernel, n_f, n_t, n_sem),
        out_shape=outs,
        in_specs=[pl.BlockSpec(memory_space=pltpu.HBM)] * 12,
        out_specs=[pl.BlockSpec(memory_space=pltpu.VMEM)] * 4,
        scratch_shapes=scratch
        + [
            pltpu.SemaphoreType.DMA((n_load,)),
            pltpu.SemaphoreType.DMA((n_sem,)),
            pltpu.SemaphoreType.DMA((n_sem,)),
        ],
        compiler_params=pltpu.CompilerParams(
            collective_id=0, has_side_effects=True, vmem_limit_bytes=34 * 1024 * 1024
        ),
        name="exchange",
    )(*(pltpu.with_memory_space_constraint(x, pltpu.HBM) for group in groups for x in group))

    cuts = 2
    specs_in, specs_out, shapes = [], [], []
    for weight, basis, moved in (
        (query_weight, query_basis, moved_query),
        (out_weight, out_basis, moved_out),
    ):
        w = moved.shape[2]
        high = weight.shape[0] // cuts
        block = pl.BlockSpec((high, w), lambda c, b, at: (b, c))
        specs_in += [
            pl.BlockSpec((high, rank), lambda c, b, at: (at[0] * cuts + b, 0)),
            pl.BlockSpec((1, rank, w), lambda c, b, at: (c, 0, 0)),
            block,
        ]
        specs_out += [block, block]
        shapes += [
            jax.ShapeDtypeStruct(weight.shape, f32),
            jax.ShapeDtypeStruct(weight.shape, bf16),
        ]
    position = lax.axis_index("fs").astype(jnp.int32).reshape(1)
    query_step, query_copy, out_step, out_copy = pl.pallas_call(
        step_kernel,
        out_shape=shapes,
        grid_spec=pltpu.PrefetchScalarGridSpec(
            num_scalar_prefetch=1, grid=(REP, cuts), in_specs=specs_in, out_specs=specs_out
        ),
        compiler_params=pltpu.CompilerParams(
            dimension_semantics=("arbitrary", "arbitrary"), vmem_limit_bytes=20 * 1024 * 1024
        ),
        name="steps",
    )(
        position,
        pltpu.with_memory_space_constraint(query_basis, pltpu.HBM), moved_query, near_query,
        pltpu.with_memory_space_constraint(out_basis, pltpu.HBM), moved_out, near_out,
    )
    return query_step, out_step, query_copy, out_copy


def solution(mesh):
    sizes = dict(mesh.shape)
    assert sizes["rep"] == REP
    placed = (
        P(("fs", "rep"), None),
        P(("fs", "rep"), "tp"),
        P(("fs", "rep"), None),
        P(("fs", "rep"), "tp"),
        P("fs", "tp"),
        P("fs", "tp"),
        P(),
        P(),
        P("fs", "tp"),
        P("fs", "tp"),
        P("fs", "tp"),
        P("fs", "tp"),
    )
    return jax.shard_map(
        functools.partial(on_device, sizes["fs"], sizes["tp"]),
        mesh=mesh,
        in_specs=placed,
        out_specs=(P("fs", "tp"), P("fs", "tp"), P("fs", "tp"), P("fs", "tp")),
        check_vma=False,
    )
```
